32 devices in a mesh: ep: 16 (over z, y, x), tp: 2 (over core).
Axes of the slice: x: 2, y: 2, z: 4, core: 2. Of those that a mesh axis runs over, the one named last changes fastest.
Arguments:
- tokens: bfloat16 [2048, 2048], P('ep'), may hold values from -6 to 6
- expert_ids: int32 [2048, 2], P('ep'), may hold values from 0 to 7, all different within a row; in each aligned block of 128 rows (0 to 127, 128 to 255, ...) at most 64 rows name the same one
- route_weights: float32 [2048, 2], P('ep'), may hold values from 0.2 to 1
- norm_gain: float32 [2048], replicated, may hold values from 0.1 to 1.9
- gate_weight: bfloat16 [2048, 8192], P(None, ('ep', 'tp')), may hold values from -0.125 to 0.125
- up_weight: bfloat16 [2048, 8192], P(None, ('ep', 'tp')), may hold values from -0.125 to 0.125
- down_weight: bfloat16 [8192, 2048], P('ep', 'tp'), may hold values from -0.1875 to 0.1875
- dense_gate: bfloat16 [2048, 256], P('ep'), may hold values from -0.125 to 0.125
- dense_up: bfloat16 [2048, 256], P('ep'), may hold values from -0.125 to 0.125
- dense_down: bfloat16 [256, 2048], P(None, 'tp'), may hold values from -0.375 to 0.375
- branch_gate: float32 [2048], P('tp'), may hold values from -3 to 3
Outputs:
- mixed: bfloat16 [2048, 2048], P('ep', 'tp')
The draws below stay inside these ranges and needn't reach their ends.
Inputs may be any that keep to these rules, and one draw needn't show every extreme that they name: `expert_ids`: each row names 2 different experts. Within the rows of one device (aligned blocks of 128 rows) no expert is named more than 64 times; in some blocks an expert is named exactly 64 times.
All inputs are finite; a program needn't handle non-finite values.
Results may differ from the reference program's by a relative error of at most 0.0074.
Values may be sent and summed in bfloat16 or wider, within the bound.
A program may use at most 64 MiB of HBM per device.

```python
import math
import jax
import jax.numpy as jnp
import numpy as np
from jax import lax

D = 2048
FF = 1024
SH = 256
TOP = 2
TOK_DEV = 128
EXPERTS = 8
TOKENS = 2048
SLOTS = 64
N_EP = 16


def levels(stream_key, dims, pieces, least, top_value):
    loudness, own = 1.0, jax.random.fold_in(stream_key, 6)
    for dim, blocks in pieces:
        heights = jnp.exp(jax.random.uniform(jax.random.fold_in(own, dim), (blocks,), jnp.float32, least / len(pieces), top_value / len(pieces)))
        loudness = loudness * jnp.repeat(heights, dims[dim] // blocks).reshape([-1 if axis == dim else 1 for axis in range(len(dims))])
    return loudness


def deal_out(key, own, number, rows, count, top, limit, skew):
    order = jax.random.permutation(key, count)
    crowded, common = portions_of(count, rows * top, limit, skew, True), portions_of(count, rows * top, limit, skew, False)
    places = jnp.arange(count)

    def named(tallies, rotation):
        used = int((tallies > 0).sum())
        fixed = max(1, used // 4)
        passed = fixed + (places - fixed + rotation * (used - fixed)) % max(1, count - fixed)
        return jnp.zeros((count,), jnp.int32).at[order[jnp.where(places < fixed, places, passed)]].set(jnp.asarray(tallies, jnp.int32))

    tallies = jnp.where(number % 4 == 0, named(crowded, number // 4), named(common, number - number // 4 - 1))
    mixed = jax.random.permutation(jax.random.fold_in(own, 3), count)
    source_of, taker = mixed[0:count // 2 * 2:2], mixed[1:count // 2 * 2:2]
    room = jnp.minimum(tallies[source_of] - 1, limit - tallies[taker]) // 2
    room = jnp.where((source_of == order[0]) | (taker == order[0]) | (tallies[taker] == 0), 0, jnp.maximum(room, 0))
    passed = jax.random.randint(jax.random.fold_in(own, 4), (count // 2,), 0, 1 << 20) % (room + 1)
    tallies = tallies.at[source_of].add(-passed).at[taker].add(passed)
    items = jnp.searchsorted(jnp.cumsum(tallies), jnp.arange(rows * top), side="right").astype(jnp.int32)
    table = items.reshape(top, rows).T
    table = table[jax.random.permutation(jax.random.fold_in(own, 1), rows)]
    rotation = jax.random.randint(jax.random.fold_in(own, 2), (rows, 1), 0, top)
    return jnp.take_along_axis(table, (jnp.arange(top)[None, :] + rotation) % top, axis=1)


def portions_of(number_of, total, bound, lean, full):
    weights = [(1 << 20) // math.isqrt(grade ** lean) + 1 for grade in range(1, number_of + 1)]
    largest = bound if full else min(bound, max(-(-total // number_of), total * weights[0] // sum(weights)))
    least = 1 if total - largest >= number_of - 1 else 0
    given, spare = [largest] + [least] * (number_of - 1), total - largest - least * (number_of - 1)
    while spare > 0:
        candidates = [i for i in range(1, number_of) if given[i] < largest] or [i for i in range(1, number_of) if given[i] < bound]
        pool, remaining = sum([weights[i] for i in candidates]), spare
        for i in candidates:
            extra = min(bound - given[i], max(1, remaining * weights[i] // pool), spare)
            given[i] = given[i] + extra
            spare = spare - extra
    return np.array(given)


def noise(own_key, shape, width, reach, pieces=(), kind=jnp.bfloat16):
    drawn = width * jax.random.normal(own_key, shape, jnp.float32)
    if pieces:
        drawn = drawn * levels(own_key, shape, pieces, -0.22, 0.18)
    return jnp.clip(drawn, -reach, reach).astype(kind)


def setup_inputs(seed: int = 0) -> dict:
    keys = jax.random.split(jax.random.key(seed), 12)
    tokens = noise(keys[0], (TOKENS, D), 1.0, 6.0, ((0, 16),))
    expert_ids_keys = jax.random.split(jax.random.fold_in(keys[1], 1), TOKENS // TOK_DEV)
    expert_ids_turns = jax.random.permutation(jax.random.fold_in(keys[1], 3), TOKENS // TOK_DEV)
    expert_ids = jax.vmap(lambda own, number: deal_out(jax.random.fold_in(keys[1], 2), own, number, TOK_DEV, EXPERTS, TOP, SLOTS, 2))(expert_ids_keys, expert_ids_turns).reshape((TOKENS, TOP))
    route_weights = jnp.clip(0.2 + 0.8 * jax.random.uniform(keys[2], (TOKENS, TOP), jnp.float32) ** levels(keys[2], (TOKENS, TOP), ((0, 16),), -0.2, 0.2), 0.2, 1.0)
    norm_gain = jnp.clip(1.0 + 0.18 * jax.random.normal(keys[3], (D,), jnp.float32), 0.1, 1.9)
    gate_weight = noise(keys[4], (D, EXPERTS * FF), D ** -0.5, 0.125, ((1, 32),))
    up_weight = noise(keys[5], (D, EXPERTS * FF), D ** -0.5, 0.125, ((1, 32),))
    down_weight = noise(keys[6], (EXPERTS * FF, D), FF ** -0.5, 0.1875, ((0, 16), (1, 2)))
    dense_gate = noise(keys[7], (D, SH), D ** -0.5, 0.125, ((0, 16),))
    dense_up = noise(keys[8], (D, SH), D ** -0.5, 0.125, ((0, 16),))
    dense_down = noise(keys[9], (SH, D), SH ** -0.5, 0.375, ((1, 2),))
    branch_gate = jnp.clip(jax.random.uniform(keys[10], (D,), jnp.float32, -3.0, 3.0) * levels(keys[10], (D,), ((0, 2),), -0.4, 0.0), -3.0, 3.0)
    return dict(tokens=tokens, expert_ids=expert_ids, route_weights=route_weights, norm_gain=norm_gain, gate_weight=gate_weight, up_weight=up_weight, down_weight=down_weight, dense_gate=dense_gate, dense_up=dense_up, dense_down=dense_down, branch_gate=branch_gate)


epsilon = 1e-06

def reference(tokens, expert_ids, route_weights, norm_gain, gate_weight, up_weight, down_weight, dense_gate, dense_up, dense_down, branch_gate):
    model_width = tokens.shape[1]
    values = tokens.astype(jnp.float32)
    inverse = lax.rsqrt(lax.optimization_barrier(jnp.mean(values * values, axis=1, keepdims=True)) + epsilon)
    normed = (values * inverse * norm_gain[None, :]).astype(jnp.bfloat16)
    dense_gate_act = jnp.dot(normed, dense_gate, preferred_element_type=jnp.float32)
    dense_up_act = jnp.dot(normed, dense_up, preferred_element_type=jnp.float32)
    dense_hidden = (jax.nn.silu(dense_gate_act) * dense_up_act).astype(jnp.bfloat16)
    dense_out = jnp.dot(dense_hidden, dense_down, preferred_element_type=jnp.float32)
    flat_ids = expert_ids.reshape(N_EP, TOK_DEV * TOP)
    labels = jnp.arange(EXPERTS, dtype=jnp.int32)
    onehot = (flat_ids[:, :, None] == labels[None, None, :]).astype(jnp.int32)
    earlier = jnp.cumsum(onehot, axis=1) - onehot
    slot_index = lax.optimization_barrier(jnp.sum(onehot * earlier, axis=2)).astype(jnp.int32)
    source = jnp.arange(N_EP, dtype=jnp.int32)[:, None]
    slot_row = (source * SLOTS + slot_index).astype(jnp.int32)
    owner_rows = (jnp.arange(TOK_DEV * TOP, dtype=jnp.int32)[None, :] // TOP + source * TOK_DEV).astype(jnp.int32)
    row_table = jnp.full((EXPERTS, N_EP * SLOTS), TOKENS, jnp.int32)
    row_table = row_table.at[flat_ids.reshape(-1), slot_row.reshape(-1)].set(owner_rows.reshape(-1))
    padded = jnp.concatenate([normed, jnp.zeros((1, model_width), jnp.bfloat16)], axis=0)
    half_width = FF // 2

    def run_expert(expert_index):
        in_rows = padded[row_table[expert_index]]
        offset = (expert_index * FF).astype(jnp.int32)
        w_gate = lax.dynamic_slice_in_dim(gate_weight, offset, FF, 1)
        w_up = lax.dynamic_slice_in_dim(up_weight, offset, FF, 1)
        w_down = lax.dynamic_slice_in_dim(down_weight, offset, FF, 0)
        expert_gate = jnp.dot(in_rows, w_gate, preferred_element_type=jnp.float32)
        expert_up = jnp.dot(in_rows, w_up, preferred_element_type=jnp.float32)
        hidden = (jax.nn.silu(expert_gate) * expert_up).astype(jnp.bfloat16)
        lower_part = jnp.dot(hidden[:, :half_width], w_down[:half_width], preferred_element_type=jnp.float32).astype(jnp.bfloat16)
        upper_part = jnp.dot(hidden[:, half_width:], w_down[half_width:], preferred_element_type=jnp.float32).astype(jnp.bfloat16)
        return (lower_part.astype(jnp.float32) + upper_part.astype(jnp.float32)).astype(jnp.bfloat16)
    results = lax.map(run_expert, jnp.arange(EXPERTS, dtype=jnp.int32))
    picked = results[flat_ids.reshape(TOKENS, TOP), slot_row.reshape(TOKENS, TOP)]
    routed = lax.optimization_barrier(jnp.sum(route_weights[:, :, None] * picked.astype(jnp.float32), axis=1))
    mixed_out = routed + jax.nn.sigmoid(branch_gate)[None, :] * dense_out
    return mixed_out.astype(jnp.bfloat16)
```

```python
import functools

import jax
import jax.numpy as jnp
from jax import lax
from jax.experimental import pallas as pl
from jax.experimental.pallas import tpu as pltpu
from jax.sharding import PartitionSpec as P

epsilon = 1e-06


def narrowed(rows):
    half_features = rows.shape[2] // 2
    return lax.dynamic_slice_in_dim(rows, lax.axis_index("tp") * half_features, half_features, 2)


def small_slot_path(
    tokens,
    expert_ids,
    route_weights,
    norm_gain,
    gate_weight,
    up_weight,
    down_weight,
    dense_gate,
    dense_up,
    dense_down,
    branch_gate,
):
    tok_rows, model_width = tokens.shape
    top_count = expert_ids.shape[1]
    ep_count = lax.axis_size("ep")
    experts = ep_count // 2
    slot_count = 2 * top_count * tok_rows // experts
    values = tokens.astype(jnp.float32)
    inverse = lax.rsqrt(jnp.mean(values * values, axis=1, keepdims=True) + epsilon)
    normed = (values * inverse * norm_gain[None, :]).astype(jnp.bfloat16)
    dense_gate_act = jnp.dot(
        normed,
        lax.all_gather(dense_gate, "ep", axis=0, tiled=True),
        preferred_element_type=jnp.float32,
    )
    dense_up_act = jnp.dot(
        normed,
        lax.all_gather(dense_up, "ep", axis=0, tiled=True),
        preferred_element_type=jnp.float32,
    )
    dense_hidden = (jax.nn.silu(dense_gate_act) * dense_up_act).astype(jnp.bfloat16)
    dense_out = jnp.dot(dense_hidden, dense_down, preferred_element_type=jnp.float32)
    flat_ids = expert_ids.reshape(tok_rows * top_count)
    labels = lax.broadcasted_iota(jnp.int32, (1, experts), 1)
    onehot = (flat_ids[:, None] == labels).astype(jnp.int32)
    earlier = jnp.cumsum(onehot, axis=0) - onehot
    slot_index = jnp.sum(onehot * earlier, axis=1)
    row_code = (flat_ids * slot_count + slot_index).reshape(tok_rows, top_count)
    targets = lax.broadcasted_iota(jnp.int32, (experts * slot_count, 1, 1), 0)
    selector = jnp.any(row_code[None, :, :] == targets, axis=2).astype(jnp.bfloat16)
    buffer = jnp.dot(selector, normed, preferred_element_type=jnp.float32).astype(jnp.bfloat16)
    buffer = buffer.reshape(experts, slot_count, model_width)
    outgoing = narrowed(jnp.repeat(buffer, 2, axis=0))
    arrived = lax.all_gather(
        lax.all_to_all(outgoing, "ep", split_axis=0, concat_axis=0, tiled=True),
        "tp",
        axis=2,
        tiled=True,
    )
    in_rows = arrived.reshape(ep_count * slot_count, model_width)
    expert_gate = jnp.dot(in_rows, gate_weight, preferred_element_type=jnp.float32)
    expert_up = jnp.dot(in_rows, up_weight, preferred_element_type=jnp.float32)
    hidden = (jax.nn.silu(expert_gate) * expert_up).astype(jnp.bfloat16)
    down_total = jnp.dot(
        lax.all_gather(hidden, "tp", axis=1, tiled=True),
        down_weight,
        preferred_element_type=jnp.float32,
    )
    partial_value = down_total.astype(jnp.bfloat16).reshape(ep_count, slot_count, -1)
    returned_rows = lax.all_to_all(partial_value, "ep", split_axis=0, concat_axis=0, tiled=True)
    pair_sums = returned_rows.reshape(experts, 2, slot_count, -1).astype(jnp.float32)
    expert_out = (
        (pair_sums[:, 0] + pair_sums[:, 1]).astype(jnp.bfloat16).reshape(experts * slot_count, -1)
    )
    picked = (
        jnp.take(expert_out, row_code.reshape(-1), axis=0)
        .reshape(tok_rows, top_count, -1)
        .astype(jnp.float32)
    )
    routed = jnp.sum(route_weights[:, :, None] * picked, axis=1)
    mixed_out = routed + jax.nn.sigmoid(branch_gate)[None, :] * dense_out
    return mixed_out.astype(jnp.bfloat16)


MESH = pl.DeviceIdType.MESH
BF16, F32 = jnp.bfloat16, jnp.float32


def flip(value, bits):
    bit = 1
    while bit <= bits:
        if bits & bit:
            value = value + bit * (1 - 2 * lax.rem(lax.div(value, bit), 2))
        bit *= 2
    return value


def expert_kernel(
    dims,
    tokens_ref,
    ids_ref,
    route_ref,
    gain_ref,
    gate_hbm,
    up_hbm,
    down_hbm,
    dense_gate_hbm,
    dense_up_hbm,
    dense_down_hbm,
    branch_ref,
    out_ref,
    normed_ref,
    outgoing,
    rows_in,
    half_own,
    half_in,
    summed,
    returned,
    w_in,
    w_out,
    dense_w,
    dense_down,
    dense_hidden,
    load_sem,
    w_send,
    w_recv,
    disp_send,
    disp_recv,
    fwd_send,
    fwd_recv,
    half_send,
    half_recv,
    ret_send,
    ret_recv,
    dense_send,
    dense_recv,
    hid_send,
    hid_recv,
):
    ep_count, experts, slot_count, top_count = dims
    share = slot_count // 2
    tok_rows, width = tokens_ref.shape
    half_width = width // 2
    dense_half = dense_hidden.shape[2]
    ep, tp = lax.axis_index("ep"), lax.axis_index("tp")
    other = 1 - tp
    side, pair = lax.rem(ep, 2), lax.div(ep, 2)
    buddy = flip(ep, 1)

    def peer(k):
        return 2 * flip(pair, k) + side

    def remote(src, dst, send, recv, device):
        return pltpu.make_async_remote_copy(
            src_ref=src, dst_ref=dst, send_sem=send, recv_sem=recv,
            device_id=device, device_id_type=MESH,
        )

    barrier = pltpu.get_barrier_semaphore()
    for k in range(experts):
        if k:
            pl.semaphore_signal(barrier, inc=1, device_id=(peer(k), tp), device_id_type=MESH)
        pl.semaphore_signal(barrier, inc=1, device_id=(peer(k), other), device_id_type=MESH)
    pl.semaphore_signal(barrier, inc=1, device_id=(buddy, tp), device_id_type=MESH)

    bit_count = ep_count.bit_length() - 1
    order = list(range(2, bit_count)) + [0, 1]
    place = 0
    for i, bit in enumerate(order):
        place = place + (1 << i) * lax.rem(lax.div(ep, 1 << bit), 2)
    dense_columns = pl.ds(pl.multiple_of(tp * dense_half, dense_half), dense_half)
    loads = [
        pltpu.make_async_copy(
            dense_gate_hbm.at[:, dense_columns], dense_w.at[place, :, pl.ds(0, dense_half)], load_sem.at[0]
        ),
        pltpu.make_async_copy(
            dense_up_hbm.at[:, dense_columns], dense_w.at[place, :, pl.ds(dense_half, dense_half)], load_sem.at[1]
        ),
        pltpu.make_async_copy(gate_hbm, w_in.at[tp, 0], load_sem.at[2]),
        pltpu.make_async_copy(up_hbm, w_in.at[tp, 1], load_sem.at[3]),
        pltpu.make_async_copy(down_hbm, w_out.at[tp], load_sem.at[4]),
        pltpu.make_async_copy(dense_down_hbm, dense_down, load_sem.at[5]),
    ]
    for load in loads:
        load.start()

    values = tokens_ref[...].astype(F32)
    inverse = lax.rsqrt(jnp.mean(values * values, axis=1, keepdims=True) + epsilon)
    normed = (values * inverse * gain_ref[...]).astype(BF16)
    normed_ref[...] = normed

    lanes = lax.broadcasted_iota(jnp.int32, (tok_rows, 128), 1)
    hits = [ids_ref[:, t : t + 1] == lanes for t in range(top_count)]
    named = sum(hit.astype(F32) for hit in hits).astype(BF16)
    lower = (
        lax.broadcasted_iota(jnp.int32, (tok_rows, tok_rows), 0)
        > lax.broadcasted_iota(jnp.int32, (tok_rows, tok_rows), 1)
    ).astype(F32).astype(BF16)
    earlier = jnp.dot(lower, named, preferred_element_type=F32)
    codes = [
        ids_ref[:, t : t + 1].astype(F32) * slot_count
        + jnp.sum(jnp.where(hits[t], earlier, 0.0), axis=1, keepdims=True)
        for t in range(top_count)
    ]

    def targets(count, per_expert, first):
        row = lax.broadcasted_iota(jnp.int32, (tok_rows, count), 1)
        expert = jnp.bitwise_xor(jnp.right_shift(row, per_expert.bit_length() - 1), pair)
        return (expert * slot_count + first + jnp.bitwise_and(row, per_expert - 1)).astype(F32)

    sent_codes = targets(experts * share, share, tp * share)
    chosen = sum((code == sent_codes).astype(F32) for code in codes)
    selector = jnp.transpose(chosen).astype(BF16)
    outgoing[...] = (
        jnp.dot(selector, normed, preferred_element_type=F32)
        .astype(BF16)
        .reshape(experts, share, width)
    )

    pl.semaphore_wait(barrier, 2 * experts)

    forwards = [
        remote(
            rows_in.at[k, 0] if k else outgoing.at[0], rows_in.at[k, 1],
            fwd_send.at[k], fwd_recv.at[k], (buddy, tp),
        )
        for k in range(experts)
    ]
    dispatches = {
        k: remote(
            outgoing.at[k], rows_in.at[k, 0], disp_send.at[k], disp_recv.at[k], (peer(k), tp)
        )
        for k in range(1, experts)
    }
    forwards[0].start()
    for k in range(1, experts):
        dispatches[k].start()
    shared = [
        remote(gate_hbm, w_in.at[tp, 0], w_send.at[0], w_recv.at[0], (ep, other)),
        remote(up_hbm, w_in.at[tp, 1], w_send.at[1], w_recv.at[1], (ep, other)),
        remote(down_hbm, w_out.at[tp], w_send.at[2], w_recv.at[2], (ep, other)),
    ]
    for copy in shared:
        copy.start()
    gathers = []
    for i, bit in enumerate(order):
        size = 1 << i
        block = dense_w.at[pl.ds(lax.div(place, size) * size, size)]
        gathers.append(
            remote(block, block, dense_send.at[i], dense_recv.at[i], (flip(ep, 1 << bit), tp))
        )

    def gathered(i):
        size = 1 << i
        block = dense_w.at[pl.ds(lax.div(flip(place, size), size) * size, size)]
        remote(block, block, dense_send.at[i], dense_recv.at[i], (ep, other)).wait_recv()

    loads[0].wait()
    loads[1].wait()
    gathers[0].start()
    rows_in[0, 0] = outgoing[0]

    def forward(group):
        for k in (2 * group, 2 * group + 1):
            if k:
                dispatches[k].wait_recv()
                forwards[k].start()

    halves = [
        remote(half_own.at[k, 1], half_in.at[k], half_send.at[k], half_recv.at[k], (buddy, tp))
        for k in range(experts)
    ]

    def compute(group):
        ks = (2 * group, 2 * group + 1)
        for k in ks:
            forwards[k].wait_recv()
        rows = rows_in[ks[0] : ks[1] + 1].reshape(4 * share, width)
        parts = []
        for core in range(2):
            gate = jnp.dot(rows, w_in[core, 0], preferred_element_type=F32)
            up = jnp.dot(rows, w_in[core, 1], preferred_element_type=F32)
            parts.append((jax.nn.silu(gate) * up).astype(BF16))
        hidden = jnp.concatenate(parts, axis=1)
        for core in range(2):
            half_own[ks[0] : ks[1] + 1, :, core] = (
                jnp.dot(hidden, w_out[core], preferred_element_type=F32)
                .astype(BF16)
                .reshape(2, 2, share, half_width)
            )
        for k in ks:
            halves[k].start()

    returns = []

    def reduce(group):
        for k in (2 * group, 2 * group + 1):
            halves[k].wait_recv()
            summed[k] = (half_own[k, 0].astype(F32) + half_in[k].astype(F32)).astype(BF16)
            for core in range(2):
                if k:
                    copy = remote(
                        summed.at[k, core], returned.at[k, tp],
                        ret_send.at[k, core], ret_recv.at[k, tp], (peer(k), core),
                    )
                elif core:
                    copy = remote(
                        summed.at[0, other], returned.at[0, tp],
                        ret_send.at[0, 1], ret_recv.at[0, tp], (ep, other),
                    )
                else:
                    returned[0, tp] = summed[0, tp]
                    continue
                copy.start()
                returns.append(copy)

    groups = experts // 2
    forward(0)
    if groups > 1:
        forward(1)
    for load in loads[2:]:
        load.wait()
    for copy in shared:
        copy.wait_recv()
    steps_done = 0

    def gather_step():
        nonlocal steps_done
        if steps_done < bit_count - 1:
            gathered(steps_done)
            steps_done += 1
            gathers[steps_done].start()

    for group in range(groups):
        if 1 <= group and group + 1 < groups:
            forward(group + 1)
        gather_step()
        compute(group)
        if group:
            reduce(group - 1)
    while steps_done < bit_count - 1:
        gather_step()
    reduce(groups - 1)
    gathered(bit_count - 1)

    dense_rows = width // ep_count
    pieces = []
    for position in range(ep_count):
        owner = sum(((position >> i) & 1) << bit for i, bit in enumerate(order))
        pieces.append(normed_ref[:, owner * dense_rows : (owner + 1) * dense_rows])
    act = jnp.dot(
        jnp.concatenate(pieces, axis=1),
        dense_w[...].reshape(width, 2 * dense_half),
        preferred_element_type=F32,
    )
    dense_hidden[tp] = (jax.nn.silu(act[:, :dense_half]) * act[:, dense_half:]).astype(BF16)
    exchange = remote(
        dense_hidden.at[tp], dense_hidden.at[tp], hid_send, hid_recv, (ep, other)
    )
    exchange.start()
    remote(
        dense_hidden.at[other], dense_hidden.at[other], hid_send, hid_recv, (ep, other)
    ).wait_recv()
    both = jnp.concatenate([dense_hidden[0], dense_hidden[1]], axis=1)
    mixed = jax.nn.sigmoid(branch_ref[...]) * jnp.dot(
        both, dense_down[...], preferred_element_type=F32
    )

    for k in range(experts):
        for core in (0, 1) if k else (other,):
            slot = returned.at[k, core]
            remote(slot, slot, ret_send.at[k, 0], ret_recv.at[k, core], (ep, other)).wait_recv()
    kept = targets(experts * slot_count, slot_count, 0)
    expert_out = returned[...].reshape(experts * slot_count, half_width)
    routed = 0.0
    for t in range(top_count):
        picker = (codes[t] == kept).astype(F32).astype(BF16)
        routed = routed + route_ref[:, t : t + 1] * jnp.dot(
            picker, expert_out, preferred_element_type=F32
        )
    out_ref[...] = (routed + mixed).astype(BF16)

    for copy in list(dispatches.values()) + forwards + shared + gathers + halves + returns + [exchange]:
        copy.wait_send()


def per_device(
    tokens,
    expert_ids,
    route_weights,
    norm_gain,
    gate_weight,
    up_weight,
    down_weight,
    dense_gate,
    dense_up,
    dense_down,
    branch_gate,
):
    tok_rows, width = tokens.shape
    top_count = expert_ids.shape[1]
    ep_count = lax.axis_size("ep")
    experts = ep_count // 2
    slot_count = 2 * top_count * tok_rows // experts
    share, dense_half = slot_count // 2, dense_gate.shape[1] // 2
    fits = (
        experts >= 4
        and experts & (experts - 1) == 0
        and slot_count & (slot_count - 1) == 0
        and share % 16 == 0
        and dense_half % 128 == 0
        and (width // ep_count) % 128 == 0
    )
    if not fits:
        return small_slot_path(
            tokens, expert_ids, route_weights, norm_gain, gate_weight, up_weight,
            down_weight, dense_gate, dense_up, dense_down, branch_gate,
        )
    half_width, columns = width // 2, gate_weight.shape[1]
    bit_count = ep_count.bit_length() - 1
    dma = pltpu.SemaphoreType.DMA
    vmem = pl.BlockSpec(memory_space=pltpu.VMEM)
    hbm = pl.BlockSpec(memory_space=pl.ANY)
    return pl.pallas_call(
        functools.partial(expert_kernel, (ep_count, experts, slot_count, top_count)),
        out_shape=jax.ShapeDtypeStruct((tok_rows, half_width), BF16),
        in_specs=[vmem] * 4 + [hbm] * 6 + [vmem],
        out_specs=vmem,
        scratch_shapes=[
            pltpu.VMEM((tok_rows, width), BF16),
            pltpu.VMEM((experts, share, width), BF16),
            pltpu.VMEM((experts, 2, share, width), BF16),
            pltpu.VMEM((experts, 2, 2, share, half_width), BF16),
            pltpu.VMEM((experts, 2, share, half_width), BF16),
            pltpu.VMEM((experts, 2, share, half_width), BF16),
            pltpu.VMEM((experts, 2, share, half_width), BF16),
            pltpu.VMEM((2, 2, width, columns), BF16),
            pltpu.VMEM((2,) + down_weight.shape, BF16),
            pltpu.VMEM((ep_count, width // ep_count, 2 * dense_half), BF16),
            pltpu.VMEM(dense_down.shape, BF16),
            pltpu.VMEM((2, tok_rows, dense_half), BF16),
            dma((6,)),
            dma((3,)),
            dma((3,)),
            dma((experts,)),
            dma((experts,)),
            dma((experts,)),
            dma((experts,)),
            dma((experts,)),
            dma((experts,)),
            dma((experts, 2)),
            dma((experts, 2)),
            dma((bit_count,)),
            dma((bit_count,)),
            dma,
            dma,
        ],
        compiler_params=pltpu.CompilerParams(
            collective_id=0, has_side_effects=True, vmem_limit_bytes=60000 * 1024
        ),
    )(
        tokens, expert_ids, route_weights, norm_gain[None, :], gate_weight, up_weight,
        down_weight, dense_gate, dense_up, dense_down, branch_gate[None, :],
    )


def solution(mesh):
    in_specs = (
        P("ep", None),
        P("ep", None),
        P("ep", None),
        P(),
        P(None, ("ep", "tp")),
        P(None, ("ep", "tp")),
        P("ep", "tp"),
        P("ep", None),
        P("ep", None),
        P(None, "tp"),
        P("tp"),
    )
    out_specs = P("ep", "tp")
    return jax.shard_map(
        per_device, mesh=mesh, in_specs=in_specs, out_specs=out_specs, check_vma=False
    )
```

```python
import functools

import jax
import jax.numpy as jnp
from jax import lax
from jax.experimental import pallas as pl
from jax.experimental.pallas import tpu as pltpu
from jax.sharding import PartitionSpec as P

epsilon = 1e-06


def narrowed(rows):
    half_features = rows.shape[2] // 2
    return lax.dynamic_slice_in_dim(rows, lax.axis_index("tp") * half_features, half_features, 2)


def small_slot_path(
    tokens,
    expert_ids,
    route_weights,
    norm_gain,
    gate_weight,
    up_weight,
    down_weight,
    dense_gate,
    dense_up,
    dense_down,
    branch_gate,
):
    tok_rows, model_width = tokens.shape
    top_count = expert_ids.shape[1]
    ep_count = lax.axis_size("ep")
    experts = ep_count // 2
    slot_count = 2 * top_count * tok_rows // experts
    values = tokens.astype(jnp.float32)
    inverse = lax.rsqrt(jnp.mean(values * values, axis=1, keepdims=True) + epsilon)
    normed = (values * inverse * norm_gain[None, :]).astype(jnp.bfloat16)
    dense_gate_act = jnp.dot(
        normed,
        lax.all_gather(dense_gate, "ep", axis=0, tiled=True),
        preferred_element_type=jnp.float32,
    )
    dense_up_act = jnp.dot(
        normed,
        lax.all_gather(dense_up, "ep", axis=0, tiled=True),
        preferred_element_type=jnp.float32,
    )
    dense_hidden = (jax.nn.silu(dense_gate_act) * dense_up_act).astype(jnp.bfloat16)
    dense_out = jnp.dot(dense_hidden, dense_down, preferred_element_type=jnp.float32)
    flat_ids = expert_ids.reshape(tok_rows * top_count)
    labels = lax.broadcasted_iota(jnp.int32, (1, experts), 1)
    onehot = (flat_ids[:, None] == labels).astype(jnp.int32)
    earlier = jnp.cumsum(onehot, axis=0) - onehot
    slot_index = jnp.sum(onehot * earlier, axis=1)
    row_code = (flat_ids * slot_count + slot_index).reshape(tok_rows, top_count)
    targets = lax.broadcasted_iota(jnp.int32, (experts * slot_count, 1, 1), 0)
    selector = jnp.any(row_code[None, :, :] == targets, axis=2).astype(jnp.bfloat16)
    buffer = jnp.dot(selector, normed, preferred_element_type=jnp.float32).astype(jnp.bfloat16)
    buffer = buffer.reshape(experts, slot_count, model_width)
    outgoing = narrowed(jnp.repeat(buffer, 2, axis=0))
    arrived = lax.all_gather(
        lax.all_to_all(outgoing, "ep", split_axis=0, concat_axis=0, tiled=True),
        "tp",
        axis=2,
        tiled=True,
    )
    in_rows = arrived.reshape(ep_count * slot_count, model_width)
    expert_gate = jnp.dot(in_rows, gate_weight, preferred_element_type=jnp.float32)
    expert_up = jnp.dot(in_rows, up_weight, preferred_element_type=jnp.float32)
    hidden = (jax.nn.silu(expert_gate) * expert_up).astype(jnp.bfloat16)
    down_total = jnp.dot(
        lax.all_gather(hidden, "tp", axis=1, tiled=True),
        down_weight,
        preferred_element_type=jnp.float32,
    )
    partial_value = down_total.astype(jnp.bfloat16).reshape(ep_count, slot_count, -1)
    returned_rows = lax.all_to_all(partial_value, "ep", split_axis=0, concat_axis=0, tiled=True)
    pair_sums = returned_rows.reshape(experts, 2, slot_count, -1).astype(jnp.float32)
    expert_out = (
        (pair_sums[:, 0] + pair_sums[:, 1]).astype(jnp.bfloat16).reshape(experts * slot_count, -1)
    )
    picked = (
        jnp.take(expert_out, row_code.reshape(-1), axis=0)
        .reshape(tok_rows, top_count, -1)
        .astype(jnp.float32)
    )
    routed = jnp.sum(route_weights[:, :, None] * picked, axis=1)
    mixed_out = routed + jax.nn.sigmoid(branch_gate)[None, :] * dense_out
    return mixed_out.astype(jnp.bfloat16)


MESH = pl.DeviceIdType.MESH
BF16, F32 = jnp.bfloat16, jnp.float32


def flip(value, bits):
    bit = 1
    while bit <= bits:
        if bits & bit:
            value = value + bit * (1 - 2 * lax.rem(lax.div(value, bit), 2))
        bit *= 2
    return value


def expert_kernel(
    dims,
    tokens_ref,
    ids_ref,
    route_ref,
    gain_ref,
    gate_hbm,
    up_hbm,
    down_hbm,
    dense_gate_hbm,
    dense_up_hbm,
    dense_down_hbm,
    branch_ref,
    out_ref,
    normed_ref,
    outgoing,
    rows_in,
    half_own,
    half_in,
    summed,
    returned,
    w_in,
    w_out,
    dense_w,
    dense_down,
    dense_hidden,
    load_sem,
    w_send,
    w_recv,
    disp_send,
    disp_recv,
    fwd_send,
    fwd_recv,
    half_send,
    half_recv,
    ret_send,
    ret_recv,
    dense_send,
    dense_recv,
    hid_send,
    hid_recv,
):
    ep_count, experts, slot_count, top_count = dims
    share = slot_count // 2
    tok_rows, width = tokens_ref.shape
    half_width = width // 2
    dense_half = dense_hidden.shape[2]
    ep, tp = lax.axis_index("ep"), lax.axis_index("tp")
    other = 1 - tp
    side, pair = lax.rem(ep, 2), lax.div(ep, 2)
    buddy = flip(ep, 1)

    def peer(k):
        return 2 * flip(pair, k) + side

    def remote(src, dst, send, recv, device):
        return pltpu.make_async_remote_copy(
            src_ref=src, dst_ref=dst, send_sem=send, recv_sem=recv,
            device_id=device, device_id_type=MESH,
        )

    barrier = pltpu.get_barrier_semaphore()
    for k in range(experts):
        if k:
            pl.semaphore_signal(barrier, inc=1, device_id=(peer(k), tp), device_id_type=MESH)
        pl.semaphore_signal(barrier, inc=1, device_id=(peer(k), other), device_id_type=MESH)
    pl.semaphore_signal(barrier, inc=1, device_id=(buddy, tp), device_id_type=MESH)

    bit_count = ep_count.bit_length() - 1
    order = list(range(2, bit_count)) + [0, 1]
    place = 0
    for i, bit in enumerate(order):
        place = place + (1 << i) * lax.rem(lax.div(ep, 1 << bit), 2)
    dense_columns = pl.ds(pl.multiple_of(tp * dense_half, dense_half), dense_half)
    loads = [
        pltpu.make_async_copy(
            dense_gate_hbm.at[:, dense_columns], dense_w.at[place, :, pl.ds(0, dense_half)], load_sem.at[0]
        ),
        pltpu.make_async_copy(
            dense_up_hbm.at[:, dense_columns], dense_w.at[place, :, pl.ds(dense_half, dense_half)], load_sem.at[1]
        ),
        pltpu.make_async_copy(gate_hbm, w_in.at[tp, 0], load_sem.at[2]),
        pltpu.make_async_copy(up_hbm, w_in.at[tp, 1], load_sem.at[3]),
        pltpu.make_async_copy(down_hbm, w_out.at[tp], load_sem.at[4]),
        pltpu.make_async_copy(dense_down_hbm, dense_down, load_sem.at[5]),
    ]
    for load in loads:
        load.start()

    values = tokens_ref[...].astype(F32)
    inverse = lax.rsqrt(jnp.mean(values * values, axis=1, keepdims=True) + epsilon)
    normed = (values * inverse * gain_ref[...]).astype(BF16)
    normed_ref[...] = normed

    lanes = lax.broadcasted_iota(jnp.int32, (tok_rows, 128), 1)
    ids = jnp.transpose(ids_ref[...].astype(F32))
    shares = jnp.transpose(route_ref[...])
    hits = [ids[:, t : t + 1].astype(jnp.int32) == lanes for t in range(top_count)]
    named = sum(hit.astype(F32) for hit in hits).astype(BF16)
    lower = (
        lax.broadcasted_iota(jnp.int32, (tok_rows, tok_rows), 0)
        > lax.broadcasted_iota(jnp.int32, (tok_rows, tok_rows), 1)
    ).astype(F32).astype(BF16)
    earlier = jnp.dot(lower, named, preferred_element_type=F32)
    codes = [
        ids[:, t : t + 1] * slot_count
        + jnp.sum(jnp.where(hits[t], earlier, 0.0), axis=1, keepdims=True)
        for t in range(top_count)
    ]

    def targets(count, per_expert, first, skipped):
        row = lax.broadcasted_iota(jnp.int32, (tok_rows, count), 1) + skipped * per_expert
        expert = jnp.bitwise_xor(jnp.right_shift(row, per_expert.bit_length() - 1), pair)
        return (expert * slot_count + first + jnp.bitwise_and(row, per_expert - 1)).astype(F32)

    sent_codes = targets(experts * share, share, tp * share, 0)
    chosen = sum((code == sent_codes).astype(F32) for code in codes)
    selector = jnp.transpose(chosen).astype(BF16)
    outgoing[...] = (
        jnp.dot(selector, normed, preferred_element_type=F32)
        .astype(BF16)
        .reshape(experts, share, width)
    )

    pl.semaphore_wait(barrier, 2 * experts)

    forwards = [
        remote(
            rows_in.at[k, 0] if k else outgoing.at[0], rows_in.at[k, 1],
            fwd_send.at[k], fwd_recv.at[k], (buddy, tp),
        )
        for k in range(experts)
    ]
    dispatches = {
        k: remote(
            outgoing.at[k], rows_in.at[k, 0], disp_send.at[k], disp_recv.at[k], (peer(k), tp)
        )
        for k in range(1, experts)
    }
    forwards[0].start()
    for k in range(1, experts):
        dispatches[k].start()
    shared = [
        remote(gate_hbm, w_in.at[tp, 0], w_send.at[0], w_recv.at[0], (ep, other)),
        remote(up_hbm, w_in.at[tp, 1], w_send.at[1], w_recv.at[1], (ep, other)),
        remote(down_hbm, w_out.at[tp], w_send.at[2], w_recv.at[2], (ep, other)),
    ]
    for copy in shared:
        copy.start()
    gathers = []
    for i, bit in enumerate(order):
        size = 1 << i
        block = dense_w.at[pl.ds(lax.div(place, size) * size, size)]
        gathers.append(
            remote(block, block, dense_send.at[i], dense_recv.at[i], (flip(ep, 1 << bit), tp))
        )

    def gathered(i):
        size = 1 << i
        block = dense_w.at[pl.ds(lax.div(flip(place, size), size) * size, size)]
        remote(block, block, dense_send.at[i], dense_recv.at[i], (ep, other)).wait_recv()

    loads[0].wait()
    loads[1].wait()
    gathers[0].start()
    rows_in[0, 0] = outgoing[0]

    def forward(k):
        if k:
            dispatches[k].wait_recv()
            forwards[k].start()

    halves = [
        remote(half_own.at[k, 1], half_in.at[k], half_send.at[k], half_recv.at[k], (buddy, tp))
        for k in range(experts)
    ]

    def compute(k):
        forwards[k].wait_recv()
        rows = rows_in[k].reshape(2 * share, width)
        parts = []
        for core in range(2):
            gate = jnp.dot(rows, w_in[core, 0], preferred_element_type=F32)
            up = jnp.dot(rows, w_in[core, 1], preferred_element_type=F32)
            parts.append((jax.nn.silu(gate) * up).astype(BF16))
        hidden = jnp.concatenate(parts, axis=1)
        for core in range(2):
            half_own[k, :, core] = (
                jnp.dot(hidden, w_out[core], preferred_element_type=F32)
                .astype(BF16)
                .reshape(2, share, half_width)
            )
        halves[k].start()

    returns = []

    def reduce(k):
        halves[k].wait_recv()
        summed[k] = (half_own[k, 0].astype(F32) + half_in[k].astype(F32)).astype(BF16)
        for core in range(2):
            if k:
                copy = remote(
                    summed.at[k, core], returned.at[k, tp],
                    ret_send.at[k, core], ret_recv.at[k, tp], (peer(k), core),
                )
            elif core:
                copy = remote(
                    summed.at[0, other], returned.at[0, tp],
                    ret_send.at[0, 1], ret_recv.at[0, tp], (ep, other),
                )
            else:
                returned[0, tp] = summed[0, tp]
                continue
            copy.start()
            returns.append(copy)

    steps_done = 0

    def gather_step():
        nonlocal steps_done
        if steps_done < bit_count - 1:
            gathered(steps_done)
            steps_done += 1
            gathers[steps_done].start()

    far = experts // 2
    compute_order = list(range(far, experts)) + list(range(far - 1, -1, -1))
    plan = [("pass", k) for k in range(far + 2)] + [("gather", 0)]
    for i, k in enumerate(compute_order):
        plan.append(("compute", k))
        if far + 2 + i < experts:
            plan.append(("pass", far + 2 + i))
        if i:
            plan.append(("send", compute_order[i - 1]))
        if i in (1, 3):
            plan.append(("gather", 0))
    weights_ready = False
    for act, k in plan:
        if act == "pass":
            forward(k)
        elif act == "gather":
            gather_step()
        elif act == "send":
            reduce(k)
        else:
            if not weights_ready:
                for load in loads[2:]:
                    load.wait()
                for copy in shared:
                    copy.wait_recv()
                weights_ready = True
            compute(k)
    while steps_done < bit_count - 1:
        gather_step()
    gathered(bit_count - 1)
    dense_rows = width // ep_count
    pieces = []
    for position in range(ep_count):
        owner = sum(((position >> i) & 1) << bit for i, bit in enumerate(order))
        pieces.append(normed_ref[:, owner * dense_rows : (owner + 1) * dense_rows])
    act = jnp.dot(
        jnp.concatenate(pieces, axis=1),
        dense_w[...].reshape(width, 2 * dense_half),
        preferred_element_type=F32,
    )
    dense_hidden[tp] = (jax.nn.silu(act[:, :dense_half]) * act[:, dense_half:]).astype(BF16)
    exchange = remote(
        dense_hidden.at[tp], dense_hidden.at[tp], hid_send, hid_recv, (ep, other)
    )
    exchange.start()
    reduce(compute_order[-1])
    remote(
        dense_hidden.at[other], dense_hidden.at[other], hid_send, hid_recv, (ep, other)
    ).wait_recv()
    both = jnp.concatenate([dense_hidden[0], dense_hidden[1]], axis=1)
    mixed = jax.nn.sigmoid(branch_ref[...]) * jnp.dot(
        both, dense_down[...], preferred_element_type=F32
    )

    routed = 0.0
    for first, last in ((2, experts), (0, 2)):
        for k in range(first, last):
            for core in (0, 1) if k else (other,):
                slot = returned.at[k, core]
                remote(slot, slot, ret_send.at[k, 0], ret_recv.at[k, core], (ep, other)).wait_recv()
        count = (last - first) * slot_count
        kept = targets(count, slot_count, 0, first)
        expert_out = returned[first:last].reshape(count, half_width)
        for t in range(top_count):
            picker = (codes[t] == kept).astype(F32).astype(BF16)
            routed = routed + shares[:, t : t + 1] * jnp.dot(
                picker, expert_out, preferred_element_type=F32
            )
    out_ref[...] = (routed + mixed).astype(BF16)

    for copy in list(dispatches.values()) + forwards + shared + gathers + halves + returns + [exchange]:
        copy.wait_send()


def per_device(
    tokens,
    expert_ids,
    route_weights,
    norm_gain,
    gate_weight,
    up_weight,
    down_weight,
    dense_gate,
    dense_up,
    dense_down,
    branch_gate,
):
    tok_rows, width = tokens.shape
    top_count = expert_ids.shape[1]
    ep_count = lax.axis_size("ep")
    experts = ep_count // 2
    slot_count = 2 * top_count * tok_rows // experts
    share, dense_half = slot_count // 2, dense_gate.shape[1] // 2
    fits = (
        experts >= 4
        and experts & (experts - 1) == 0
        and slot_count & (slot_count - 1) == 0
        and share % 16 == 0
        and dense_half % 128 == 0
        and (width // ep_count) % 128 == 0
    )
    if not fits:
        return small_slot_path(
            tokens, expert_ids, route_weights, norm_gain, gate_weight, up_weight,
            down_weight, dense_gate, dense_up, dense_down, branch_gate,
        )
    half_width, columns = width // 2, gate_weight.shape[1]
    bit_count = ep_count.bit_length() - 1
    dma = pltpu.SemaphoreType.DMA
    vmem = pl.BlockSpec(memory_space=pltpu.VMEM)
    hbm = pl.BlockSpec(memory_space=pl.ANY)
    return pl.pallas_call(
        functools.partial(expert_kernel, (ep_count, experts, slot_count, top_count)),
        out_shape=jax.ShapeDtypeStruct((tok_rows, half_width), BF16),
        in_specs=[vmem] * 4 + [hbm] * 6 + [vmem],
        out_specs=vmem,
        scratch_shapes=[
            pltpu.VMEM((tok_rows, width), BF16),
            pltpu.VMEM((experts, share, width), BF16),
            pltpu.VMEM((experts, 2, share, width), BF16),
            pltpu.VMEM((experts, 2, 2, share, half_width), BF16),
            pltpu.VMEM((experts, 2, share, half_width), BF16),
            pltpu.VMEM((experts, 2, share, half_width), BF16),
            pltpu.VMEM((experts, 2, share, half_width), BF16),
            pltpu.VMEM((2, 2, width, columns), BF16),
            pltpu.VMEM((2,) + down_weight.shape, BF16),
            pltpu.VMEM((ep_count, width // ep_count, 2 * dense_half), BF16),
            pltpu.VMEM(dense_down.shape, BF16),
            pltpu.VMEM((2, tok_rows, dense_half), BF16),
            dma((6,)),
            dma((3,)),
            dma((3,)),
            dma((experts,)),
            dma((experts,)),
            dma((experts,)),
            dma((experts,)),
            dma((experts,)),
            dma((experts,)),
            dma((experts, 2)),
            dma((experts, 2)),
            dma((bit_count,)),
            dma((bit_count,)),
            dma,
            dma,
        ],
        compiler_params=pltpu.CompilerParams(
            collective_id=0, has_side_effects=True, vmem_limit_bytes=60000 * 1024
        ),
    )(
        tokens, expert_ids.T, route_weights.T, norm_gain[None, :], gate_weight, up_weight,
        down_weight, dense_gate, dense_up, dense_down, branch_gate[None, :],
    )


def solution(mesh):
    in_specs = (
        P("ep", None),
        P("ep", None),
        P("ep", None),
        P(),
        P(None, ("ep", "tp")),
        P(None, ("ep", "tp")),
        P("ep", "tp"),
        P("ep", None),
        P("ep", None),
        P(None, "tp"),
        P("tp"),
    )
    out_specs = P("ep", "tp")
    return jax.shard_map(
        per_device, mesh=mesh, in_specs=in_specs, out_specs=out_specs, check_vma=False
    )
```
